32 devices in a mesh: grp: 2 (over y), sp: 4 (over z), dp: 4 (over x, core).
Axes of the slice: x: 2, y: 2, z: 4, core: 2. Of those that a mesh axis runs over, the one named last changes fastest.
Arguments:
- gate_input: bfloat16 [8, 1536, 2048], P(('grp', 'dp'), 'sp'), parts along dimension 0, may hold values from -6 to 6
- value_input: bfloat16 [8, 1536, 2048], P(('grp', 'dp'), 'sp'), parts along dimension 0, may hold values from -6 to 6
- norm_gain: bfloat16 [2048], replicated, may hold values from 0.099609375 to 1.8984375
- norm_bias: bfloat16 [2048], replicated, may hold values from -2.5 to 2.5
- mix_weight: bfloat16 [16, 1024, 1024], P('sp', 'dp'), may hold values from -0.1875 to 0.1875
- mix_bias: bfloat16 [16, 1024], P('sp'), may hold values from 0.099609375 to 1.8984375
Outputs:
- gated: bfloat16 [8, 1536, 2048], P(('grp', 'dp'), 'sp'), parts along dimension 0
The draws below stay inside these ranges and needn't reach their ends.
There are 2 independent parts, one for each index of `grp`. The reference program is written for one: setup_inputs(seed, part) draws one part's arguments, and reference() takes and returns one part's arrays. A program takes and returns all parts, laid end to end along the dimension named above; an argument that names none is the same for every part. Nothing has to cross between parts.
All inputs are finite; a program needn't handle non-finite values.
Results may differ from the reference program's by a relative error of at most 0.0053.
Values may be sent and summed in bfloat16 or wider, within the bound.
No kernel may reach another device: no remote copies, remote signals or barrier semaphores. Data moves between devices by JAX's collectives and lax.ppermute only.
A program may use at most 64 MiB of HBM per device.

```python
import jax
import jax.numpy as jnp
from jax import lax

GD = 128
G = 16
GW = 2048
BLK = 1024
LEN = 1536
SEQS = 4


def level_of(rng, dims, cuts, low, top_value):
    gain = 1.0
    for position, shards_of in cuts:
        draws = jax.random.uniform(jax.random.fold_in(jax.random.fold_in(rng, 6), position), (shards_of,), jnp.float32, low / len(cuts), top_value / len(cuts))
        gain = gain * jnp.repeat(jnp.exp(draws), dims[position] // shards_of).reshape((-1,) + (1,) * (len(dims) - 1 - position))
    return gain


def gaussian(stream_key, dims, deviation, limit, pieces=(), held_as=jnp.bfloat16):
    values = deviation * jax.random.normal(stream_key, dims, jnp.float32)
    if pieces:
        values = values * level_of(stream_key, dims, pieces, -0.22, 0.18)
    return jnp.clip(values, -limit, limit).astype(held_as)


def setup_inputs(seed: int = 0, part: int = 0) -> dict:
    key_of = jax.random.split(jax.random.key(seed), 7)
    part_keys = jax.random.split(jax.random.fold_in(key_of[6], part), 7)
    gate_input = gaussian(part_keys[0], (SEQS, LEN, GW), 1.0, 6.0, ((0, 4), (1, 4)))
    value_input = gaussian(part_keys[1], (SEQS, LEN, GW), 1.0, 6.0, ((0, 4), (1, 4)))
    norm_gain = jnp.clip(1.0 + 0.18 * jax.random.normal(key_of[2], (GW,), jnp.float32), 0.099609375, 1.8984375).astype(jnp.bfloat16)
    norm_bias = gaussian(key_of[3], (GW,), 0.5, 2.5)
    mix_weight = gaussian(key_of[4], (G, BLK, BLK), BLK ** -0.5, 0.1875, ((0, 4), (1, 4)))
    mix_bias = jnp.clip(1.0 + 0.18 * jax.random.normal(key_of[5], (G, BLK), jnp.float32), 0.099609375, 1.8984375).astype(jnp.bfloat16)
    return {"gate_input": gate_input, "value_input": value_input, "norm_gain": norm_gain, "norm_bias": norm_bias, "mix_weight": mix_weight, "mix_bias": mix_bias}


def reference(gate_input, value_input, norm_gain, norm_bias, mix_weight, mix_bias):
    seqs, length, width = value_input.shape
    nblocks = -(-length // BLK)
    act = jax.nn.gelu(value_input.astype(jnp.float32))
    mean = lax.optimization_barrier(jnp.mean(act, axis=-1, keepdims=True))
    var = lax.optimization_barrier(jnp.mean(jnp.square(act - mean), axis=-1, keepdims=True))
    normed = ((act - mean) * lax.rsqrt(var + 1e-06) * norm_gain.astype(jnp.float32) + norm_bias.astype(jnp.float32)).astype(jnp.bfloat16)
    keep = jnp.tril(jnp.ones((BLK, BLK), dtype=bool))
    weight_full = jnp.where(keep[None], mix_weight.astype(jnp.float32), jnp.float32(0.0))
    bias_full = mix_bias.astype(jnp.float32).T[None, :, :, None]

    def mix_sequence(normed_seq):
        padded = jnp.pad(normed_seq, ((0, nblocks * BLK - length), (0, 0)))
        blocks = padded.reshape(nblocks, BLK, G, GD).astype(jnp.float32)
        mixed = jnp.einsum('gts,bsgc->btgc', weight_full, blocks) + bias_full
        return mixed.reshape(nblocks * BLK, width)[:length].astype(jnp.bfloat16)
    mixed = lax.map(mix_sequence, normed)
    mixed = lax.optimization_barrier(mixed)
    gated = jax.nn.gelu(gate_input.astype(jnp.float32)) * mixed.astype(jnp.float32)
    return gated.astype(jnp.bfloat16)
```

```python
import functools

import jax
import jax.numpy as jnp
from jax import lax
from jax.experimental import pallas as pl
from jax.experimental.pallas import tpu as pltpu
from jax.sharding import PartitionSpec as P


GD = 128
BLK = 1024
TILE = 256


VMEM = pl.BlockSpec(memory_space=pltpu.VMEM)
SMEM = pl.BlockSpec(memory_space=pltpu.SMEM)


def gelu(x):
    half = 0.5 * x
    return half + half * jnp.tanh(x * (0.7978845608028654 + 0.035677408136300125 * (x * x)))


def norm_kernel(shards, chunks, width, rows_step, at_ref, x_ref, gain_ref, bias_ref, *refs):
    outs, held = refs[:-1], refs[-1]
    here = at_ref[0]
    span = chunks * width
    gain = gain_ref[...].astype(jnp.float32)
    bias = bias_ref[...].astype(jnp.float32)

    def step(i, carry):
        rows = pl.ds(pl.multiple_of(i * rows_step, rows_step), rows_step)
        act = gelu(x_ref[rows, :].astype(jnp.float32))
        centred = act - jnp.mean(act, axis=-1, keepdims=True)
        var = jnp.mean(jnp.square(centred), axis=-1, keepdims=True)
        held[rows, :] = (centred * lax.rsqrt(var + 1e-06) * gain + bias).astype(jnp.bfloat16)
        return carry

    steps = x_ref.shape[0] // rows_step
    lax.fori_loop(0, steps, step, 0, unroll=4 if steps % 4 == 0 else 1)
    for c in range(chunks):
        for s in range(shards):
            owner = lax.rem(here + s, shards)
            start = pl.multiple_of(owner * span + c * width, GD)
            outs[c * shards + s][...] = held[:, pl.ds(start, width)]


def mix_kernel(shards, length, first, layout, at_ref, *refs):
    pieces, refs = refs[:shards], refs[shards:]
    weights, refs = refs[:len(layout)], refs[len(layout):]
    bias_ref, outs, (values, mixed) = refs[0], refs[1:1 + shards], refs[1 + shards:]
    here, row = at_ref[0], at_ref[1]
    rows = pieces[0].shape[0]
    groups = pieces[0].shape[1] // GD
    nblocks = -(-length // BLK)
    for s in range(shards):
        origin = lax.rem(here + shards - s, shards)
        mixed[pl.ds(pl.multiple_of(origin * rows, rows), rows), :] = pieces[s][...]
    for g in range(groups):
        for b in range(nblocks):
            count = min(BLK, length - b * BLK)
            lanes = pl.ds(b * GD, GD)
            values[g, pl.ds(0, count), lanes] = mixed[pl.ds(b * BLK, count), pl.ds(g * GD, GD)]
            if count < BLK:
                values[g, pl.ds(count, BLK - count), lanes] = jnp.zeros((BLK - count, GD), jnp.bfloat16)
    tiles = {}
    for ref, (flip, first_row, low) in zip(weights, layout):
        tiles.setdefault((flip, first_row), []).append((ref, low))
    for (flip, first_row), parts in tiles.items():
        at_row = row ^ flip if first_row is None else first_row
        top = pl.multiple_of(at_row * TILE, TILE)
        for g in range(groups):
            total = None
            for ref, low in parts:
                if first_row is None:
                    part = ref[g]
                else:
                    part = ref[g, pl.ds(first_row * TILE, TILE), :]
                cols = lax.broadcasted_iota(jnp.int32, part.shape, 1) + low
                keep = cols <= lax.broadcasted_iota(jnp.int32, part.shape, 0) + top
                part = jnp.where(keep, part, jnp.zeros_like(part))
                term = jnp.dot(part, values[g, pl.ds(low, part.shape[1]), :], preferred_element_type=jnp.float32)
                total = term if total is None else total + term
            total = total + bias_ref[pl.ds(top, TILE), pl.ds(first + g, 1)]
            for b in range(nblocks):
                mixed[pl.ds(b * BLK + top, TILE), pl.ds(g * GD, GD)] = total[:, b * GD:(b + 1) * GD].astype(jnp.bfloat16)
    for s in range(shards):
        target = lax.rem(here + s, shards)
        outs[s][...] = mixed[pl.ds(pl.multiple_of(target * rows, rows), rows), :]


def gate_kernel(shards, at_ref, gate_ref, *refs):
    pieces, out_ref = refs[:shards], refs[-1]
    for s in range(shards):

        @pl.when(pl.program_id(0) == s)
        def _():
            gate = gelu(gate_ref[...].astype(jnp.float32))
            out_ref[...] = (gate * pieces[s][...].astype(jnp.float32)).astype(jnp.bfloat16)


def shift_pairs(count, by):
    return [(i, (i + by) % count) for i in range(count)]


def flip_pairs(count, by):
    return [(i, i ^ by) for i in range(count)]


def exchange_rows(parts, ndp):
    got = []
    whole = parts[0]
    got.append((whole, 0, None, 0))
    got.append((lax.ppermute(whole, "dp", flip_pairs(ndp, 1)), 1, None, 0))
    for low, least, part in parts[1:]:
        far = lax.ppermute(part, "dp", [p for p in flip_pairs(ndp, 2) if p[0] >= least])
        got.append((far, 2, None, low))
        got.append((lax.ppermute(far, "dp", flip_pairs(ndp, 1)), 3, None, low))
    return got


def gathered_rows(weight):
    whole = lax.all_gather(weight, "dp", axis=1, tiled=True)
    return [(whole, 0, i, 0) for i in range(BLK // TILE)]


def compute(nsp, ndp, exchange, gate, value, gain, bias, mix_weight, bias_rows):
    rows, width = value.shape
    groups = mix_weight.shape[0]
    length = rows * nsp
    chunks = 2 if groups % 2 == 0 else 1
    per = groups // chunks
    rows_step = 16
    nblocks = -(-length // BLK)
    at = jnp.stack([lax.axis_index("sp").astype(jnp.int32), lax.axis_index("dp").astype(jnp.int32)])
    piece = jax.ShapeDtypeStruct((rows, per * GD), jnp.bfloat16)

    weights = []
    for c in range(chunks):
        own = lax.slice_in_dim(mix_weight, c * per, (c + 1) * per, axis=0)
        if exchange:
            cuts = [(0, 2 * TILE, 0), (2 * TILE, TILE, 2), (3 * TILE, TILE, 3)]
            parts = [(low, least, lax.slice_in_dim(own, low, low + count, axis=2)) for low, count, least in cuts]
            weights.append(exchange_rows([own] + parts, ndp))
        else:
            weights.append(gathered_rows(own))

    sent = pl.pallas_call(
        functools.partial(norm_kernel, nsp, chunks, per * GD, rows_step),
        out_shape=[piece] * (nsp * chunks),
        in_specs=[SMEM, VMEM, VMEM, VMEM],
        out_specs=[VMEM] * (nsp * chunks),
        scratch_shapes=[pltpu.VMEM((rows, width), jnp.bfloat16)],
        cost_estimate=pl.CostEstimate(flops=30 * rows * width, bytes_accessed=4 * rows * width, transcendentals=rows * width),
        name="norm",
    )(at, value, gain, bias)
    out = None
    got = []
    for c in range(chunks):
        mine = sent[c * nsp:(c + 1) * nsp]
        got.append([mine[0]] + [lax.ppermute(mine[s], "sp", shift_pairs(nsp, s)) for s in range(1, nsp)])
    for c in range(chunks):
        layout = [(flip, fixed, low) for _, flip, fixed, low in weights[c]]
        outs = pl.pallas_call(
            functools.partial(mix_kernel, nsp, length, c * per, layout),
            out_shape=[piece] * nsp,
            in_specs=[SMEM] + [VMEM] * (nsp + len(layout) + 1),
            out_specs=[VMEM] * nsp,
            scratch_shapes=[
                pltpu.VMEM((per, BLK, nblocks * GD), jnp.bfloat16),
                pltpu.VMEM((nblocks * BLK, per * GD), jnp.bfloat16),
            ],
            cost_estimate=pl.CostEstimate(flops=2 * per * BLK * length * GD, bytes_accessed=per * BLK * BLK, transcendentals=0),
        )(at, *got[c], *[w[0] for w in weights[c]], bias_rows)
        back = [outs[0]] + [lax.ppermute(outs[s], "sp", shift_pairs(nsp, s)) for s in range(1, nsp)]

        def block(s, at_ref, c=c):
            return 0, lax.rem(at_ref[0] + nsp - s, nsp) * chunks + c

        wide = pl.BlockSpec((rows, per * GD), block)
        extra = [] if out is None else [out]
        out = pl.pallas_call(
            functools.partial(gate_kernel, nsp),
            out_shape=jax.ShapeDtypeStruct((rows, width), jnp.bfloat16),
            grid_spec=pltpu.PrefetchScalarGridSpec(
                num_scalar_prefetch=1,
                grid=(nsp,),
                in_specs=[wide] + [VMEM] * nsp + [pl.BlockSpec(memory_space=pl.ANY)] * len(extra),
                out_specs=wide,
            ),
            input_output_aliases={nsp + 2: 0} if extra else {},
            cost_estimate=pl.CostEstimate(flops=12 * rows * width // chunks, bytes_accessed=6 * rows * width // chunks, transcendentals=rows * width // chunks),
        )(at, gate, *back, *extra)
    return out


def body(nsp, ndp, exchange, gate_input, value_input, norm_gain, norm_bias, mix_weight, mix_bias):
    seqs, _, width = value_input.shape
    gain = norm_gain.reshape(1, width)
    bias = norm_bias.reshape(1, width)
    bias_rows = mix_bias.astype(jnp.float32).T
    return jnp.stack([
        compute(nsp, ndp, exchange, gate_input[q], value_input[q], gain, bias, mix_weight, bias_rows)
        for q in range(seqs)
    ])


def solution(mesh):
    nsp, ndp = mesh.shape["sp"], mesh.shape["dp"]
    exchange = ndp == BLK // TILE == 4
    placed = (
        P(("grp", "dp"), "sp", None),
        P(("grp", "dp"), "sp", None),
        P(),
        P(),
        P("sp", "dp", None),
        P("sp", None),
    )
    return jax.shard_map(
        functools.partial(body, nsp, ndp, exchange),
        mesh=mesh,
        in_specs=placed,
        out_specs=P(("grp", "dp"), "sp", None),
        check_vma=False,
    )
```

```python
import functools

import jax
import jax.numpy as jnp
from jax import lax
from jax.experimental import pallas as pl
from jax.experimental.pallas import tpu as pltpu
from jax.sharding import PartitionSpec as P


GD = 128
BLK = 1024
TILE = 256


VMEM = pl.BlockSpec(memory_space=pltpu.VMEM)
HBM = pl.BlockSpec(memory_space=pltpu.HBM)


def gelu(x):
    half = 0.5 * x
    return half + half * jnp.tanh(x * (0.7978845608028654 + 0.035677408136300125 * (x * x)))


def partner(here, step, shards):
    if shards & (shards - 1) == 0:
        return here ^ step, here ^ step
    return lax.rem(here + step, shards), lax.rem(here + shards - step, shards)


def swap_pairs(count, step):
    if count & (count - 1) == 0:
        return [(i, i ^ step) for i in range(count)]
    return [(i, (i + step) % count) for i in range(count)]


def steps_of(shards):
    return list(range(shards - 1, 0, -1))


def norm_kernel(shards, chunks, width, rows_step, cuts, value_ref, gain_ref, bias_ref, weight_ref, *refs):
    nouts = shards * chunks
    outs, parts = refs[:nouts], refs[nouts:nouts + len(cuts)]
    value, gain, bias, held, sems = refs[nouts + len(cuts):]
    here = lax.axis_index("sp")
    span = chunks * width
    rows = value.shape[0]
    loads = 3 if rows % (3 * rows_step) == 0 else 1
    block = rows // loads
    pairs = [(value_ref.at[pl.ds(0, block), :], value.at[pl.ds(0, block), :]), (gain_ref, gain), (bias_ref, bias)]
    pairs += [(value_ref.at[pl.ds(k * block, block), :], value.at[pl.ds(k * block, block), :]) for k in range(1, loads)]
    for part, (first, count, low, cols) in zip(parts, cuts):
        pairs.append((weight_ref.at[pl.ds(first, count), :, pl.ds(low, cols)], part))
    copies = [pltpu.make_async_copy(source, target, sems.at[k]) for k, (source, target) in enumerate(pairs)]
    for copy in copies:
        copy.start()
    for k in range(loads):
        if k == 0:
            for copy in copies[:3]:
                copy.wait()
            scale = gain[...].astype(jnp.float32).reshape(1, -1)
            offset = bias[...].astype(jnp.float32).reshape(1, -1)
        else:
            copies[2 + k].wait()

        def step(i, carry, k=k):
            at = pl.ds(pl.multiple_of(k * block + i * rows_step, rows_step), rows_step)
            act = gelu(value[at, :].astype(jnp.float32))
            centred = act - jnp.mean(act, axis=-1, keepdims=True)
            var = jnp.mean(jnp.square(centred), axis=-1, keepdims=True)
            held[at, :] = (centred * lax.rsqrt(var + 1e-06) * scale + offset).astype(jnp.bfloat16)
            return carry

        steps = block // rows_step
        lax.fori_loop(0, steps, step, 0, unroll=8 if steps % 8 == 0 else 1)
        at = pl.ds(k * block, block)
        for c in range(chunks):
            for s in range(shards):
                start = pl.multiple_of(partner(here, s, shards)[0] * span + c * width, GD)
                outs[c * shards + s][at, :] = held[at, pl.ds(start, width)]
    for copy in copies[2 + loads:]:
        copy.wait()


def mix_kernel(shards, length, first, layout, *refs):
    pieces, refs = refs[:shards], refs[shards:]
    weights, refs = refs[:len(layout)], refs[len(layout):]
    bias_ref, outs, (values, mixed) = refs[0], refs[1:1 + shards], refs[1 + shards:]
    here, row = lax.axis_index("sp"), lax.axis_index("dp")
    rows = pieces[0].shape[0]
    groups = pieces[0].shape[1] // GD
    nblocks = -(-length // BLK)
    for s in range(shards):
        origin = partner(here, s, shards)[1]
        mixed[pl.ds(pl.multiple_of(origin * rows, rows), rows), :] = pieces[s][...]
    for g in range(groups):
        for b in range(nblocks):
            count = min(BLK, length - b * BLK)
            lanes = pl.ds(b * GD, GD)
            values[g, pl.ds(0, count), lanes] = mixed[pl.ds(b * BLK, count), pl.ds(g * GD, GD)]
            if count < BLK:
                values[g, pl.ds(count, BLK - count), lanes] = jnp.zeros((BLK - count, GD), jnp.bfloat16)
    tiles = {}
    for ref, (flip, fixed, low, skip) in zip(weights, layout):
        tiles.setdefault((flip, fixed), []).append((ref, low, skip))
    for (flip, fixed), parts in tiles.items():
        at_row = row ^ flip if fixed is None else fixed
        top = pl.multiple_of(at_row * TILE, TILE)
        for g in range(groups):
            total = None
            for ref, low, skip in parts:
                part = ref[skip + g] if fixed is None else ref[skip + g, pl.ds(fixed * TILE, TILE), :]
                cols = lax.broadcasted_iota(jnp.int32, part.shape, 1) + low
                keep = cols <= lax.broadcasted_iota(jnp.int32, part.shape, 0) + top
                part = jnp.where(keep, part, jnp.zeros_like(part))
                term = jnp.dot(part, values[g, pl.ds(low, part.shape[1]), :], preferred_element_type=jnp.float32)
                total = term if total is None else total + term
            shift = bias_ref[pl.ds(first + g, 1), pl.ds(top, TILE)].astype(jnp.float32)
            shift = jnp.broadcast_to(shift, (GD, TILE)).T
            for b in range(nblocks):
                block = total[:, b * GD:(b + 1) * GD] + shift
                mixed[pl.ds(b * BLK + top, TILE), pl.ds(g * GD, GD)] = block.astype(jnp.bfloat16)
    for s in range(shards):
        target = partner(here, s, shards)[0]
        outs[s][...] = mixed[pl.ds(pl.multiple_of(target * rows, rows), rows), :]


def gate_kernel(shards, chunks, chunk, rows_step, gate_ref, *refs):
    pieces = refs[:shards]
    out_ref, held, sems = refs[-3:]
    here = lax.axis_index("sp")
    width = pieces[0].shape[1]
    copies = []
    for s in range(shards):
        start = (partner(here, s, shards)[1] * chunks + chunk) * width
        lanes = pl.ds(pl.multiple_of(start, GD), width)

        def step(i, carry, s=s, lanes=lanes):
            rows = pl.ds(pl.multiple_of(i * rows_step, rows_step), rows_step)
            gate = gelu(gate_ref[rows, lanes].astype(jnp.float32))
            held[s, rows, :] = (gate * pieces[s][rows, :].astype(jnp.float32)).astype(jnp.bfloat16)
            return carry

        lax.fori_loop(0, gate_ref.shape[0] // rows_step, step, 0, unroll=4)
        copies.append(pltpu.make_async_copy(held.at[s], out_ref.at[:, lanes], sems.at[s]))
        copies[-1].start()
    for copy in copies:
        copy.wait()


def exchange_rows(weight, parts, ndp, first):
    got = [(weight[0], 0, None, 0, first), (weight[1], 1, None, 0, first)]
    for low, least, part in parts:
        far = lax.ppermute(part, "dp", [p for p in swap_pairs(ndp, 2) if p[0] >= least])
        got.append((far, 2, None, low, 0))
        got.append((lax.ppermute(far, "dp", swap_pairs(ndp, 1)), 3, None, low, 0))
    return got


def compute(nsp, ndp, exchange, gate, value, gain, bias, mix_weight, mix_bias):
    rows, width = value.shape
    groups = mix_weight.shape[0]
    length = rows * nsp
    chunks = 2 if groups % 2 == 0 else 1
    per = groups // chunks
    nblocks = -(-length // BLK)
    piece = jax.ShapeDtypeStruct((rows, per * GD), jnp.bfloat16)
    small = pltpu.CompilerParams(vmem_limit_bytes=16 << 20)

    columns = [(0, 2 * TILE, 0), (2 * TILE, TILE, 2), (3 * TILE, TILE, 3)] if exchange else []
    cuts = [(c * per, per, low, cols) for c in range(chunks) for low, cols, _ in columns]
    made = pl.pallas_call(
        functools.partial(norm_kernel, nsp, chunks, per * GD, 16, cuts),
        out_shape=[piece] * (nsp * chunks)
        + [jax.ShapeDtypeStruct((n, mix_weight.shape[1], cols), jnp.bfloat16) for _, n, _, cols in cuts],
        in_specs=[HBM] * 4,
        out_specs=[VMEM] * (nsp * chunks + len(cuts)),
        scratch_shapes=[
            pltpu.VMEM((rows, width), jnp.bfloat16),
            pltpu.VMEM((width,), jnp.bfloat16),
            pltpu.VMEM((width,), jnp.bfloat16),
            pltpu.VMEM((rows, width), jnp.bfloat16),
            pltpu.SemaphoreType.DMA((5 + len(cuts),)),
        ],
        compiler_params=small,
        cost_estimate=pl.CostEstimate(flops=30 * rows * width, bytes_accessed=4 * rows * width, transcendentals=rows * width),
        name="norm",
    )(*[pltpu.with_memory_space_constraint(x, pltpu.HBM) for x in (value, gain, bias, mix_weight)])
    sent, parts = made[:nsp * chunks], made[nsp * chunks:]
    weights = []
    if exchange:
        other = lax.ppermute(mix_weight, "dp", swap_pairs(ndp, 1))
        for c in range(chunks):
            mine = parts[c * len(columns):(c + 1) * len(columns)]
            mine = [(low, least, part) for (low, _, least), part in zip(columns, mine)]
            weights.append(exchange_rows((mix_weight, other), mine, ndp, c * per))
    else:
        whole = lax.all_gather(mix_weight, "dp", axis=1, tiled=True)
        weights = [[(whole, 0, i, 0, c * per) for i in range(BLK // TILE)] for c in range(chunks)]
    out = None
    got = []
    for c in range(chunks):
        mine = sent[c * nsp:(c + 1) * nsp]
        far = {s: lax.ppermute(mine[s], "sp", swap_pairs(nsp, s)) for s in steps_of(nsp)}
        got.append([mine[0]] + [far[s] for s in range(1, nsp)])
    backs = []
    for c in range(chunks):
        layout = [w[1:] for w in weights[c]]
        outs = pl.pallas_call(
            functools.partial(mix_kernel, nsp, length, c * per, layout),
            out_shape=[piece] * nsp,
            in_specs=[VMEM] * (nsp + len(layout) + 1),
            out_specs=[VMEM] * nsp,
            scratch_shapes=[
                pltpu.VMEM((per, BLK, nblocks * GD), jnp.bfloat16),
                pltpu.VMEM((nblocks * BLK, per * GD), jnp.bfloat16),
            ],
            compiler_params=pltpu.CompilerParams(vmem_limit_bytes=24 << 20),
            cost_estimate=pl.CostEstimate(flops=2 * per * BLK * length * GD, bytes_accessed=per * BLK * BLK, transcendentals=0),
        )(*got[c], *[w[0] for w in weights[c]], mix_bias)
        far = {s: lax.ppermute(outs[s], "sp", swap_pairs(nsp, s)) for s in steps_of(nsp)}
        backs += [[outs[0]] + [far[s] for s in range(1, nsp)]]
    out = None
    for c in range(chunks):
        extra = [] if out is None else [out]
        out = pl.pallas_call(
            functools.partial(gate_kernel, nsp, chunks, c, 32),
            out_shape=jax.ShapeDtypeStruct((rows, width), jnp.bfloat16),
            in_specs=[VMEM] * (1 + nsp) + [HBM] * len(extra),
            out_specs=HBM,
            scratch_shapes=[pltpu.VMEM((nsp, rows, per * GD), jnp.bfloat16), pltpu.SemaphoreType.DMA((nsp,))],
            input_output_aliases={nsp + 1: 0} if extra else {},
            compiler_params=small,
            cost_estimate=pl.CostEstimate(flops=12 * rows * width // chunks, bytes_accessed=6 * rows * width // chunks, transcendentals=rows * width // chunks),
        )(gate, *backs[c], *extra)
    return out


def body(nsp, ndp, exchange, gate_input, value_input, norm_gain, norm_bias, mix_weight, mix_bias):
    outs = [
        compute(nsp, ndp, exchange, gate_input[q], value_input[q], norm_gain, norm_bias, mix_weight, mix_bias)
        for q in range(value_input.shape[0])
    ]
    return jnp.stack(outs)


def solution(mesh):
    nsp, ndp = mesh.shape["sp"], mesh.shape["dp"]
    exchange = ndp == BLK // TILE == 4
    placed = (
        P(("grp", "dp"), "sp", None),
        P(("grp", "dp"), "sp", None),
        P(),
        P(),
        P("sp", "dp", None),
        P("sp", None),
    )
    return jax.shard_map(
        functools.partial(body, nsp, ndp, exchange),
        mesh=mesh,
        in_specs=placed,
        out_specs=P(("grp", "dp"), "sp", None),
        check_vma=False,
    )
```

```python
import functools

import jax
import jax.numpy as jnp
from jax import lax
from jax.experimental import pallas as pl
from jax.experimental.pallas import tpu as pltpu
from jax.sharding import PartitionSpec as P


GD = 128
BLK = 1024
TILE = 256


VMEM = pl.BlockSpec(memory_space=pltpu.VMEM)
HBM = pl.BlockSpec(memory_space=pltpu.HBM)


def twice_gelu(x):
    return x + x * jnp.tanh(x * (0.7978845608028654 + 0.035677408136300125 * (x * x)))


def partner(here, step, shards):
    if shards & (shards - 1) == 0:
        return here ^ step, here ^ step
    return lax.rem(here + step, shards), lax.rem(here + shards - step, shards)


def swap_pairs(count, step):
    if count & (count - 1) == 0:
        return [(i, i ^ step) for i in range(count)]
    return [(i, (i + step) % count) for i in range(count)]


def steps_of(shards):
    return list(range(shards - 1, 0, -1))


def normalise(value, held, scale, offset, rows_step):
    def step(i, carry):
        at = pl.ds(pl.multiple_of(i * rows_step, rows_step), rows_step)
        act = twice_gelu(value[at, :].astype(jnp.float32))
        centred = act - jnp.mean(act, axis=-1, keepdims=True)
        var = jnp.mean(jnp.square(centred), axis=-1, keepdims=True)
        held[at, :] = (centred * lax.rsqrt(var + 4e-06) * scale + offset).astype(jnp.bfloat16)
        return carry

    steps = value.shape[0] // rows_step
    lax.fori_loop(0, steps, step, 0, unroll=8 if steps % 8 == 0 else 1)


def hand_out(shards, span, lanes, held, outs):
    here = lax.axis_index("sp")
    for out, (s, low, width) in zip(outs, lanes):
        start = pl.multiple_of(partner(here, s, shards)[0] * span + low, GD)
        out[...] = held[:, pl.ds(start, width)]


def weight_copies(cuts, weight_ref, parts, sems, first):
    copies = []
    for k, (part, (group, count, low, cols)) in enumerate(zip(parts, cuts)):
        source = weight_ref.at[pl.ds(group, count), :, pl.ds(low, cols)]
        copies.append(pltpu.make_async_copy(source, part, sems.at[first + k]))
    return copies


def head_kernel(shards, span, rows_step, lanes, cuts, value_ref, gain_ref, bias_ref, weight_ref, *refs):
    outs, parts = refs[:len(lanes)], refs[len(lanes):len(lanes) + len(cuts)]
    rest, gain, bias, value, held, sems = refs[len(lanes) + len(cuts):]
    head = value.shape[0]
    pairs = [
        (value_ref.at[pl.ds(0, head), :], value),
        (gain_ref, gain),
        (bias_ref, bias),
        (value_ref.at[pl.ds(head, rest.shape[0]), :], rest),
    ]
    copies = [pltpu.make_async_copy(source, target, sems.at[k]) for k, (source, target) in enumerate(pairs)]
    copies += weight_copies(cuts, weight_ref, parts, sems, len(pairs))
    for copy in copies:
        copy.start()
    for copy in copies[:3]:
        copy.wait()
    scale = gain[...].astype(jnp.float32).reshape(1, -1)
    offset = bias[...].astype(jnp.float32).reshape(1, -1)
    normalise(value, held, scale, offset, rows_step)
    hand_out(shards, span, lanes, held, outs)
    for copy in copies[3:]:
        copy.wait()


def rest_kernel(shards, span, rows_step, lanes, cuts, value, gain, bias, weight_ref, *refs):
    outs, parts = refs[:len(lanes)], refs[len(lanes):len(lanes) + len(cuts)]
    held, sems = refs[len(lanes) + len(cuts):]
    copies = weight_copies(cuts, weight_ref, parts, sems, 0)
    for copy in copies:
        copy.start()
    scale = gain[...].astype(jnp.float32).reshape(1, -1)
    offset = bias[...].astype(jnp.float32).reshape(1, -1)
    normalise(value, held, scale, offset, rows_step)
    hand_out(shards, span, lanes, held, outs)
    for copy in copies:
        copy.wait()


def mix_kernel(shards, length, first, start, layout, *refs):
    early, pieces, refs = refs[:shards], refs[shards:2 * shards], refs[2 * shards:]
    weights, refs = refs[:len(layout)], refs[len(layout):]
    bias_ref, outs, (values, mixed) = refs[0], refs[1:1 + shards], refs[1 + shards:]
    here, row = lax.axis_index("sp"), lax.axis_index("dp")
    head = early[0].shape[0]
    rest = pieces[0].shape[0]
    rows = head + rest
    groups = pieces[0].shape[1] // GD
    nblocks = -(-length // BLK)
    for s in range(shards):
        origin = partner(here, s, shards)[1]
        top = pl.multiple_of(origin * rows, GD)
        mixed[pl.ds(top, head), :] = early[s][:, pl.ds(start, groups * GD)]
        mixed[pl.ds(top + head, rest), :] = pieces[s][...]
    for g in range(groups):
        for b in range(nblocks):
            count = min(BLK, length - b * BLK)
            lanes = pl.ds(b * GD, GD)
            values[g, pl.ds(0, count), lanes] = mixed[pl.ds(b * BLK, count), pl.ds(g * GD, GD)]
            if count < BLK:
                values[g, pl.ds(count, BLK - count), lanes] = jnp.zeros((BLK - count, GD), jnp.bfloat16)
    tiles = {}
    for ref, (flip, fixed, low, skip) in zip(weights, layout):
        tiles.setdefault((flip, fixed), []).append((ref, low, skip))
    for (flip, fixed), parts in tiles.items():
        at_row = row ^ flip if fixed is None else fixed
        top = pl.multiple_of(at_row * TILE, TILE)
        for g in range(groups):
            total = None
            for ref, low, skip in parts:
                part = ref[skip + g] if fixed is None else ref[skip + g, pl.ds(fixed * TILE, TILE), :]
                cols = lax.broadcasted_iota(jnp.int32, part.shape, 1) + low
                keep = cols <= lax.broadcasted_iota(jnp.int32, part.shape, 0) + top
                part = jnp.where(keep, part, jnp.zeros_like(part))
                term = jnp.dot(part, values[g, pl.ds(low, part.shape[1]), :], preferred_element_type=jnp.float32)
                total = term if total is None else total + term
            shift = bias_ref[pl.ds(first + g, 1), pl.ds(top, TILE)].astype(jnp.float32)
            shift = jnp.broadcast_to(shift, (GD, TILE)).T
            for b in range(nblocks):
                block = total[:, b * GD:(b + 1) * GD] + shift
                mixed[pl.ds(b * BLK + top, TILE), pl.ds(g * GD, GD)] = block.astype(jnp.bfloat16)
    for s in range(shards):
        target = partner(here, s, shards)[0]
        outs[s][...] = mixed[pl.ds(pl.multiple_of(target * rows, rows), rows), :]


def gate_kernel(shards, chunks, chunk, steps, rows_step, gate_ref, *refs):
    pieces = refs[:len(steps)]
    out_ref, held, sems = refs[-3:]
    here = lax.axis_index("sp")
    width = pieces[0].shape[1]
    copies = []
    for k, s in enumerate(steps):
        start = (partner(here, s, shards)[1] * chunks + chunk) * width
        lanes = pl.ds(pl.multiple_of(start, GD), width)

        def step(i, carry, k=k, lanes=lanes):
            rows = pl.ds(pl.multiple_of(i * rows_step, rows_step), rows_step)
            gate = 0.5 * twice_gelu(gate_ref[rows, lanes].astype(jnp.float32))
            held[k, rows, :] = (gate * pieces[k][rows, :].astype(jnp.float32)).astype(jnp.bfloat16)
            return carry

        lax.fori_loop(0, gate_ref.shape[0] // rows_step, step, 0, unroll=4)
        copies.append(pltpu.make_async_copy(held.at[k], out_ref.at[:, lanes], sems.at[k]))
        copies[-1].start()
    for copy in copies:
        copy.wait()


def exchange_step(step, x, shards):
    return lax.ppermute(x, "sp", swap_pairs(shards, step))


def exchange_rows(weight, parts, ndp, first):
    got = [(weight[0], 0, None, 0, first), (weight[1], 1, None, 0, first)]
    for low, least, part in parts:
        far = lax.ppermute(part, "dp", [p for p in swap_pairs(ndp, 2) if p[0] >= least])
        got.append((far, 2, None, low, 0))
        got.append((lax.ppermute(far, "dp", swap_pairs(ndp, 1)), 3, None, low, 0))
    return got


def compute(nsp, ndp, exchange, gate, value, gain, bias, mix_weight, mix_bias):
    rows, width = value.shape
    groups = mix_weight.shape[0]
    length = rows * nsp
    chunks = 2 if groups % 2 == 0 else 1
    per = groups // chunks
    nblocks = -(-length // BLK)
    piece = jax.ShapeDtypeStruct((rows, per * GD), jnp.bfloat16)
    small = pltpu.CompilerParams(vmem_limit_bytes=16 << 20)

    columns = [(0, 2 * TILE, 0), (2 * TILE, TILE, 2), (3 * TILE, TILE, 3)] if exchange else []
    cuts = [(c * per, per, low, cols) for c in range(chunks) for low, cols, _ in columns]
    head = rows // 3
    span = groups * GD

    ncuts = len(cuts) // 2

    def bf16(*shape):
        return jax.ShapeDtypeStruct(shape, jnp.bfloat16)

    def cut_shapes(some):
        return [bf16(n, mix_weight.shape[1], cols) for _, n, _, cols in some]

    def cost(count):
        return pl.CostEstimate(flops=30 * count * width, bytes_accessed=4 * count * width, transcendentals=count * width)

    in_hbm = [pltpu.with_memory_space_constraint(x, pltpu.HBM) for x in (value, gain, bias, mix_weight)]
    lanes = [(s, 0, span) for s in range(nsp)]
    shapes = [bf16(head, span)] * nsp + cut_shapes(cuts[:ncuts]) + [bf16(rows - head, width), bf16(width), bf16(width)]
    made = pl.pallas_call(
        functools.partial(head_kernel, nsp, span, 16, lanes, cuts[:ncuts]),
        out_shape=shapes,
        in_specs=[HBM] * 4,
        out_specs=[VMEM] * len(shapes),
        scratch_shapes=[
            pltpu.VMEM((head, width), jnp.bfloat16),
            pltpu.VMEM((head, width), jnp.bfloat16),
            pltpu.SemaphoreType.DMA((4 + ncuts,)),
        ],
        compiler_params=small,
        cost_estimate=cost(head),
        name="norm_head",
    )(*in_hbm)
    first_sent, parts, ready = made[:nsp], made[nsp:nsp + ncuts], made[nsp + ncuts:]
    far = {s: exchange_step(s, first_sent[s], nsp) for s in steps_of(nsp)}
    early = [first_sent[0]] + [far[s] for s in range(1, nsp)]
    lanes = [(s, c * per * GD, per * GD) for c in range(chunks) for s in range(nsp)]
    shapes = [bf16(rows - head, per * GD)] * (nsp * chunks) + cut_shapes(cuts[ncuts:])
    made = pl.pallas_call(
        functools.partial(rest_kernel, nsp, span, 16, lanes, cuts[ncuts:]),
        out_shape=shapes,
        in_specs=[VMEM] * 3 + [HBM],
        out_specs=[VMEM] * len(shapes),
        scratch_shapes=[
            pltpu.VMEM((rows - head, width), jnp.bfloat16),
            pltpu.SemaphoreType.DMA((max(1, ncuts),)),
        ],
        compiler_params=small,
        cost_estimate=cost(rows - head),
        name="norm_rest",
    )(*ready, in_hbm[3])
    sent, parts = made[:nsp * chunks], list(parts) + list(made[nsp * chunks:])
    weights = []
    if exchange:
        other = lax.ppermute(mix_weight, "dp", swap_pairs(ndp, 1))
        for c in range(chunks):
            mine = parts[c * len(columns):(c + 1) * len(columns)]
            mine = [(low, least, part) for (low, _, least), part in zip(columns, mine)]
            weights.append(exchange_rows((mix_weight, other), mine, ndp, c * per))
    else:
        whole = lax.all_gather(mix_weight, "dp", axis=1, tiled=True)
        weights = [[(whole, 0, i, 0, c * per) for i in range(BLK // TILE)] for c in range(chunks)]
    out = None
    got = []
    for c in range(chunks):
        mine = sent[c * nsp:(c + 1) * nsp]
        far = {s: exchange_step(s, mine[s], nsp) for s in steps_of(nsp)}
        got.append([mine[0]] + [far[s] for s in range(1, nsp)])
    backs = []
    for c in range(chunks):
        layout = [w[1:] for w in weights[c]]
        outs = pl.pallas_call(
            functools.partial(mix_kernel, nsp, length, c * per, c * per * GD, layout),
            out_shape=[piece] * nsp,
            in_specs=[VMEM] * (2 * nsp + len(layout) + 1),
            out_specs=[VMEM] * nsp,
            scratch_shapes=[
                pltpu.VMEM((per, BLK, nblocks * GD), jnp.bfloat16),
                pltpu.VMEM((nblocks * BLK, per * GD), jnp.bfloat16),
            ],
            compiler_params=pltpu.CompilerParams(vmem_limit_bytes=24 << 20),
            cost_estimate=pl.CostEstimate(flops=2 * per * BLK * length * GD, bytes_accessed=per * BLK * BLK, transcendentals=0),
        )(*early, *got[c], *[w[0] for w in weights[c]], mix_bias)
        far = {s: exchange_step(s, outs[s], nsp) for s in steps_of(nsp)}
        backs += [[outs[0]] + [far[s] for s in range(1, nsp)]]
    out = None
    order = list(range(nsp))
    calls = [(c, order) for c in range(chunks - 1)] + [(chunks - 1, order[:-1]), (chunks - 1, order[-1:])]
    for c, steps in calls:
        extra = [] if out is None else [out]
        share = rows * per * GD * len(steps)
        out = pl.pallas_call(
            functools.partial(gate_kernel, nsp, chunks, c, steps, 32),
            out_shape=jax.ShapeDtypeStruct((rows, width), jnp.bfloat16),
            in_specs=[VMEM] * (1 + len(steps)) + [HBM] * len(extra),
            out_specs=HBM,
            scratch_shapes=[pltpu.VMEM((len(steps), rows, per * GD), jnp.bfloat16), pltpu.SemaphoreType.DMA((len(steps),))],
            input_output_aliases={len(steps) + 1: 0} if extra else {},
            compiler_params=small,
            cost_estimate=pl.CostEstimate(flops=12 * share, bytes_accessed=6 * share, transcendentals=share),
        )(gate, *[backs[c][s] for s in steps], *extra)
    return out


def body(nsp, ndp, exchange, gate_input, value_input, norm_gain, norm_bias, mix_weight, mix_bias):
    outs = [
        compute(nsp, ndp, exchange, gate_input[q], value_input[q], norm_gain, norm_bias, mix_weight, mix_bias)
        for q in range(value_input.shape[0])
    ]
    return jnp.stack(outs)


def solution(mesh):
    nsp, ndp = mesh.shape["sp"], mesh.shape["dp"]
    exchange = ndp == BLK // TILE == 4
    placed = (
        P(("grp", "dp"), "sp", None),
        P(("grp", "dp"), "sp", None),
        P(),
        P(),
        P("sp", "dp", None),
        P("sp", None),
    )
    return jax.shard_map(
        functools.partial(body, nsp, ndp, exchange),
        mesh=mesh,
        in_specs=placed,
        out_specs=P(("grp", "dp"), "sp", None),
        check_vma=False,
    )
```

```python
import functools

import jax
import jax.numpy as jnp
from jax import lax
from jax.experimental import pallas as pl
from jax.experimental.pallas import tpu as pltpu
from jax.sharding import PartitionSpec as P


GD = 128
BLK = 1024
TILE = 256


VMEM = pl.BlockSpec(memory_space=pltpu.VMEM)
HBM = pl.BlockSpec(memory_space=pltpu.HBM)


def twice_gelu(x):
    return x + x * jnp.tanh(x * (0.7978845608028654 + 0.035677408136300125 * (x * x)))


def partner(here, step, shards):
    if shards & (shards - 1) == 0:
        return here ^ step, here ^ step
    return lax.rem(here + step, shards), lax.rem(here + shards - step, shards)


def swap_pairs(count, step):
    if count & (count - 1) == 0:
        return [(i, i ^ step) for i in range(count)]
    return [(i, (i + step) % count) for i in range(count)]


def steps_of(shards):
    return list(range(shards - 1, 0, -1))


def normalise(value, held, scale, offset, rows_step):
    def step(i, carry):
        at = pl.ds(pl.multiple_of(i * rows_step, rows_step), rows_step)
        act = twice_gelu(value[at, :].astype(jnp.float32))
        centred = act - jnp.mean(act, axis=-1, keepdims=True)
        var = jnp.mean(jnp.square(centred), axis=-1, keepdims=True)
        held[at, :] = (centred * lax.rsqrt(var + 4e-06) * scale + offset).astype(jnp.bfloat16)
        return carry

    steps = value.shape[0] // rows_step
    lax.fori_loop(0, steps, step, 0, unroll=next(u for u in (8, 6, 4, 1) if steps % u == 0))


def hand_out(shards, span, lanes, held, outs):
    here = lax.axis_index("sp")
    for out, (s, low, width) in zip(outs, lanes):
        start = pl.multiple_of(partner(here, s, shards)[0] * span + low, GD)
        out[...] = held[:, pl.ds(start, width)]


def weight_copies(cuts, weight_ref, parts, sems, first):
    copies = []
    for k, (part, (group, count, low, cols)) in enumerate(zip(parts, cuts)):
        source = weight_ref.at[pl.ds(group, count), :, pl.ds(low, cols)]
        copies.append(pltpu.make_async_copy(source, part, sems.at[first + k]))
    return copies


def head_kernel(shards, span, rows_step, lanes, cuts, value_ref, gain_ref, bias_ref, weight_ref, *refs):
    outs, parts = refs[:len(lanes)], refs[len(lanes):len(lanes) + len(cuts)]
    rest, gain, bias, value, held, sems = refs[len(lanes) + len(cuts):]
    head = value.shape[0]
    half = head // 2
    pairs = [
        (value_ref.at[pl.ds(0, half), :], value.at[pl.ds(0, half), :]),
        (gain_ref, gain),
        (bias_ref, bias),
        (value_ref.at[pl.ds(half, head - half), :], value.at[pl.ds(half, head - half), :]),
        (value_ref.at[pl.ds(head, rest.shape[0]), :], rest),
    ]
    copies = [pltpu.make_async_copy(source, target, sems.at[k]) for k, (source, target) in enumerate(pairs)]
    copies += weight_copies(cuts, weight_ref, parts, sems, len(pairs))
    for copy in copies:
        copy.start()
    for copy in copies[:3]:
        copy.wait()
    scale = gain[...].astype(jnp.float32).reshape(1, -1)
    offset = bias[...].astype(jnp.float32).reshape(1, -1)
    normalise(value.at[pl.ds(0, half), :], held.at[pl.ds(0, half), :], scale, offset, rows_step)
    copies[3].wait()
    normalise(value.at[pl.ds(half, head - half), :], held.at[pl.ds(half, head - half), :], scale, offset, rows_step)
    hand_out(shards, span, lanes, held, outs)
    for copy in copies[4:]:
        copy.wait()


def rest_kernel(shards, span, rows_step, lanes, cuts, value, gain, bias, weight_ref, *refs):
    outs, parts = refs[:len(lanes)], refs[len(lanes):len(lanes) + len(cuts)]
    held, sems = refs[len(lanes) + len(cuts):]
    copies = weight_copies(cuts, weight_ref, parts, sems, 0)
    for copy in copies:
        copy.start()
    scale = gain[...].astype(jnp.float32).reshape(1, -1)
    offset = bias[...].astype(jnp.float32).reshape(1, -1)
    normalise(value, held, scale, offset, rows_step)
    hand_out(shards, span, lanes, held, outs)
    for copy in copies:
        copy.wait()


def mix_kernel(shards, length, first, start, layout, *refs):
    early, pieces, refs = refs[:shards], refs[shards:2 * shards], refs[2 * shards:]
    weights, refs = refs[:len(layout)], refs[len(layout):]
    bias_ref, outs, (values, mixed) = refs[0], refs[1:1 + shards], refs[1 + shards:]
    here, row = lax.axis_index("sp"), lax.axis_index("dp")
    head = early[0].shape[0]
    rest = pieces[0].shape[0]
    rows = head + rest
    groups = pieces[0].shape[1] // GD
    nblocks = -(-length // BLK)
    for s in range(shards):
        origin = partner(here, s, shards)[1]
        top = pl.multiple_of(origin * rows, GD)
        mixed[pl.ds(top, head), :] = early[s][:, pl.ds(start, groups * GD)]
        mixed[pl.ds(top + head, rest), :] = pieces[s][...]
    for g in range(groups):
        for b in range(nblocks):
            count = min(BLK, length - b * BLK)
            lanes = pl.ds(b * GD, GD)
            values[g, pl.ds(0, count), lanes] = mixed[pl.ds(b * BLK, count), pl.ds(g * GD, GD)]
            if count < BLK:
                values[g, pl.ds(count, BLK - count), lanes] = jnp.zeros((BLK - count, GD), jnp.bfloat16)
    tiles = {}
    for ref, (flip, fixed, low, skip) in zip(weights, layout):
        tiles.setdefault((flip, fixed), []).append((ref, low, skip))
    for (flip, fixed), parts in tiles.items():
        at_row = row ^ flip if fixed is None else fixed
        top = pl.multiple_of(at_row * TILE, TILE)
        for g in range(groups):
            total = None
            for ref, low, skip in parts:
                part = ref[skip + g] if fixed is None else ref[skip + g, pl.ds(fixed * TILE, TILE), :]
                cols = lax.broadcasted_iota(jnp.int32, part.shape, 1) + low
                keep = cols <= lax.broadcasted_iota(jnp.int32, part.shape, 0) + top
                part = jnp.where(keep, part, jnp.zeros_like(part))
                term = jnp.dot(part, values[g, pl.ds(low, part.shape[1]), :], preferred_element_type=jnp.float32)
                total = term if total is None else total + term
            shift = bias_ref[pl.ds(first + g, 1), pl.ds(top, TILE)].astype(jnp.float32)
            shift = jnp.broadcast_to(shift, (GD, TILE)).T
            for b in range(nblocks):
                block = total[:, b * GD:(b + 1) * GD] + shift
                mixed[pl.ds(b * BLK + top, TILE), pl.ds(g * GD, GD)] = block.astype(jnp.bfloat16)
    for s in range(shards):
        target = partner(here, s, shards)[0]
        outs[s][...] = mixed[pl.ds(pl.multiple_of(target * rows, rows), rows), :]


def gate_kernel(shards, chunks, chunk, steps, rows_step, gate_ref, *refs):
    pieces = refs[:len(steps)]
    out_ref, held, sems = refs[-3:]
    here = lax.axis_index("sp")
    width = pieces[0].shape[1]
    copies = []
    parts = sems.shape[1]
    block = gate_ref.shape[0] // parts
    for k, s in enumerate(steps):
        start = (partner(here, s, shards)[1] * chunks + chunk) * width
        lanes = pl.ds(pl.multiple_of(start, GD), width)

        for part in range(parts):

            def step(i, carry, k=k, part=part, lanes=lanes):
                rows = pl.ds(pl.multiple_of(part * block + i * rows_step, rows_step), rows_step)
                gate = 0.5 * twice_gelu(gate_ref[rows, lanes].astype(jnp.float32))
                held[k, rows, :] = (gate * pieces[k][rows, :].astype(jnp.float32)).astype(jnp.bfloat16)
                return carry

            lax.fori_loop(0, block // rows_step, step, 0, unroll=4)
            rows = pl.ds(part * block, block)
            copies.append(pltpu.make_async_copy(held.at[k, rows, :], out_ref.at[rows, lanes], sems.at[k, part]))
            copies[-1].start()
    for copy in copies:
        copy.wait()


def exchange_step(step, x, shards):
    return lax.ppermute(x, "sp", swap_pairs(shards, step))


def exchange_rows(weight, parts, ndp, first):
    got = [(weight[0], 0, None, 0, first), (weight[1], 1, None, 0, first)]
    for low, least, part in parts:
        far = lax.ppermute(part, "dp", [p for p in swap_pairs(ndp, 2) if p[0] >= least])
        got.append((far, 2, None, low, 0))
        got.append((lax.ppermute(far, "dp", swap_pairs(ndp, 1)), 3, None, low, 0))
    return got


def compute(nsp, ndp, exchange, gate, value, gain, bias, mix_weight, mix_bias):
    rows, width = value.shape
    groups = mix_weight.shape[0]
    length = rows * nsp
    chunks = 2 if groups % 2 == 0 else 1
    per = groups // chunks
    nblocks = -(-length // BLK)
    piece = jax.ShapeDtypeStruct((rows, per * GD), jnp.bfloat16)
    small = pltpu.CompilerParams(vmem_limit_bytes=16 << 20)

    columns = [(0, 2 * TILE, 0), (2 * TILE, TILE, 2), (3 * TILE, TILE, 3)] if exchange else []
    cuts = [(c * per, per, low, cols) for c in range(chunks) for low, cols, _ in columns]
    head = rows // 3
    span = groups * GD

    ncuts = len(cuts) // 2

    def bf16(*shape):
        return jax.ShapeDtypeStruct(shape, jnp.bfloat16)

    def cut_shapes(some):
        return [bf16(n, mix_weight.shape[1], cols) for _, n, _, cols in some]

    def cost(count):
        return pl.CostEstimate(flops=30 * count * width, bytes_accessed=4 * count * width, transcendentals=count * width)

    in_hbm = [pltpu.with_memory_space_constraint(x, pltpu.HBM) for x in (value, gain, bias, mix_weight)]
    lanes = [(s, 0, span) for s in range(nsp)]
    shapes = [bf16(head, span)] * nsp + cut_shapes(cuts[:ncuts]) + [bf16(rows - head, width), bf16(width), bf16(width)]
    made = pl.pallas_call(
        functools.partial(head_kernel, nsp, span, 16, lanes, cuts[:ncuts]),
        out_shape=shapes,
        in_specs=[HBM] * 4,
        out_specs=[VMEM] * len(shapes),
        scratch_shapes=[
            pltpu.VMEM((head, width), jnp.bfloat16),
            pltpu.VMEM((head, width), jnp.bfloat16),
            pltpu.SemaphoreType.DMA((5 + ncuts,)),
        ],
        compiler_params=small,
        cost_estimate=cost(head),
        name="norm_head",
    )(*in_hbm)
    first_sent, parts, ready = made[:nsp], made[nsp:nsp + ncuts], made[nsp + ncuts:]
    far = {s: exchange_step(s, first_sent[s], nsp) for s in steps_of(nsp)}
    early = [first_sent[0]] + [far[s] for s in range(1, nsp)]
    lanes = [(s, c * per * GD, per * GD) for c in range(chunks) for s in range(nsp)]
    shapes = [bf16(rows - head, per * GD)] * (nsp * chunks) + cut_shapes(cuts[ncuts:])
    made = pl.pallas_call(
        functools.partial(rest_kernel, nsp, span, 16, lanes, cuts[ncuts:]),
        out_shape=shapes,
        in_specs=[VMEM] * 3 + [HBM],
        out_specs=[VMEM] * len(shapes),
        scratch_shapes=[
            pltpu.VMEM((rows - head, width), jnp.bfloat16),
            pltpu.SemaphoreType.DMA((max(1, ncuts),)),
        ],
        compiler_params=small,
        cost_estimate=cost(rows - head),
        name="norm_rest",
    )(*ready, in_hbm[3])
    sent, parts = made[:nsp * chunks], list(parts) + list(made[nsp * chunks:])
    weights = []
    if exchange:
        other = lax.ppermute(mix_weight, "dp", swap_pairs(ndp, 1))
        for c in range(chunks):
            mine = parts[c * len(columns):(c + 1) * len(columns)]
            mine = [(low, least, part) for (low, _, least), part in zip(columns, mine)]
            weights.append(exchange_rows((mix_weight, other), mine, ndp, c * per))
    else:
        whole = lax.all_gather(mix_weight, "dp", axis=1, tiled=True)
        weights = [[(whole, 0, i, 0, c * per) for i in range(BLK // TILE)] for c in range(chunks)]
    out = None
    got = []
    for c in range(chunks):
        mine = sent[c * nsp:(c + 1) * nsp]
        far = {s: exchange_step(s, mine[s], nsp) for s in steps_of(nsp)}
        got.append([mine[0]] + [far[s] for s in range(1, nsp)])
    backs = []
    for c in range(chunks):
        layout = [w[1:] for w in weights[c]]
        outs = pl.pallas_call(
            functools.partial(mix_kernel, nsp, length, c * per, c * per * GD, layout),
            out_shape=[piece] * nsp,
            in_specs=[VMEM] * (2 * nsp + len(layout) + 1),
            out_specs=[VMEM] * nsp,
            scratch_shapes=[
                pltpu.VMEM((per, BLK, nblocks * GD), jnp.bfloat16),
                pltpu.VMEM((nblocks * BLK, per * GD), jnp.bfloat16),
            ],
            compiler_params=pltpu.CompilerParams(vmem_limit_bytes=24 << 20),
            cost_estimate=pl.CostEstimate(flops=2 * per * BLK * length * GD, bytes_accessed=per * BLK * BLK, transcendentals=0),
        )(*early, *got[c], *[w[0] for w in weights[c]], mix_bias)
        far = {s: exchange_step(s, outs[s], nsp) for s in steps_of(nsp)}
        backs += [[outs[0]] + [far[s] for s in range(1, nsp)]]
    out = None
    order = list(range(nsp))
    calls = [(c, order) for c in range(chunks - 1)] + [(chunks - 1, order[:-1]), (chunks - 1, order[-1:])]
    for c, steps in calls:
        extra = [] if out is None else [out]
        share = rows * per * GD * len(steps)
        out = pl.pallas_call(
            functools.partial(gate_kernel, nsp, chunks, c, steps, 32),
            out_shape=jax.ShapeDtypeStruct((rows, width), jnp.bfloat16),
            in_specs=[VMEM] * (1 + len(steps)) + [HBM] * len(extra),
            out_specs=HBM,
            scratch_shapes=[pltpu.VMEM((len(steps), rows, per * GD), jnp.bfloat16), pltpu.SemaphoreType.DMA((len(steps), 3 if rows % 96 == 0 else 1))],
            input_output_aliases={len(steps) + 1: 0} if extra else {},
            compiler_params=small,
            cost_estimate=pl.CostEstimate(flops=12 * share, bytes_accessed=6 * share, transcendentals=share),
        )(gate, *[backs[c][s] for s in steps], *extra)
    return out


def body(nsp, ndp, exchange, gate_input, value_input, norm_gain, norm_bias, mix_weight, mix_bias):
    outs = [
        compute(nsp, ndp, exchange, gate_input[q], value_input[q], norm_gain, norm_bias, mix_weight, mix_bias)
        for q in range(value_input.shape[0])
    ]
    return jnp.stack(outs)


def solution(mesh):
    nsp, ndp = mesh.shape["sp"], mesh.shape["dp"]
    exchange = ndp == BLK // TILE == 4
    placed = (
        P(("grp", "dp"), "sp", None),
        P(("grp", "dp"), "sp", None),
        P(),
        P(),
        P("sp", "dp", None),
        P("sp", None),
    )
    return jax.shard_map(
        functools.partial(body, nsp, ndp, exchange),
        mesh=mesh,
        in_specs=placed,
        out_specs=P(("grp", "dp"), "sp", None),
        check_vma=False,
    )
```

```python
import functools

import jax
import jax.numpy as jnp
from jax import lax
from jax.experimental import pallas as pl
from jax.experimental.pallas import tpu as pltpu
from jax.sharding import PartitionSpec as P


GD = 128
BLK = 1024
TILE = 256


VMEM = pl.BlockSpec(memory_space=pltpu.VMEM)
HBM = pl.BlockSpec(memory_space=pltpu.HBM)


def twice_gelu(x):
    return x + x * jnp.tanh(x * (0.7978845608028654 + 0.035677408136300125 * (x * x)))


def partner(here, step, shards):
    if shards & (shards - 1) == 0:
        return here ^ step, here ^ step
    return lax.rem(here + step, shards), lax.rem(here + shards - step, shards)


def swap_pairs(count, step):
    if count & (count - 1) == 0:
        return [(i, i ^ step) for i in range(count)]
    return [(i, (i + step) % count) for i in range(count)]


def steps_of(shards):
    return list(range(shards - 1, 0, -1))


def normalise(value, held, scale, offset, rows_step):
    def step(i, carry):
        at = pl.ds(pl.multiple_of(i * rows_step, rows_step), rows_step)
        act = twice_gelu(value[at, :].astype(jnp.float32))
        centred = act - jnp.mean(act, axis=-1, keepdims=True)
        var = jnp.mean(jnp.square(centred), axis=-1, keepdims=True)
        held[at, :] = (centred * lax.rsqrt(var + 4e-06) * scale + offset).astype(jnp.bfloat16)
        return carry

    steps = value.shape[0] // rows_step
    lax.fori_loop(0, steps, step, 0, unroll=next(u for u in (8, 9, 7, 6, 5, 4, 3, 2, 1) if steps % u == 0))


def hand_out(shards, span, lanes, held, outs):
    here = lax.axis_index("sp")
    for out, (s, low, width) in zip(outs, lanes):
        start = pl.multiple_of(partner(here, s, shards)[0] * span + low, GD)
        out[...] = held[:, pl.ds(start, width)]


def weight_copies(cuts, weight_ref, parts, sems, first):
    copies = []
    for k, (part, (group, count, low, cols)) in enumerate(zip(parts, cuts)):
        source = weight_ref.at[pl.ds(group, count), :, pl.ds(low, cols)]
        copies.append(pltpu.make_async_copy(source, part, sems.at[first + k]))
    return copies


def head_kernel(shards, span, rows_step, lanes, cuts, value_ref, gain_ref, bias_ref, weight_ref, *refs):
    outs, parts = refs[:len(lanes)], refs[len(lanes):len(lanes) + len(cuts)]
    gain, bias, value, held, sems = refs[len(lanes) + len(cuts):]
    head = value.shape[0]
    half = head // 32 * 16
    pairs = [
        (value_ref.at[pl.ds(0, half), :], value.at[pl.ds(0, half), :]),
        (gain_ref, gain),
        (bias_ref, bias),
        (value_ref.at[pl.ds(half, head - half), :], value.at[pl.ds(half, head - half), :]),
    ]
    copies = [pltpu.make_async_copy(source, target, sems.at[k]) for k, (source, target) in enumerate(pairs)]
    copies += weight_copies(cuts, weight_ref, parts, sems, len(pairs))
    for copy in copies:
        copy.start()
    for copy in copies[:3]:
        copy.wait()
    scale = gain[...].astype(jnp.float32).reshape(1, -1)
    offset = bias[...].astype(jnp.float32).reshape(1, -1)
    normalise(value.at[pl.ds(0, half), :], held.at[pl.ds(0, half), :], scale, offset, rows_step)
    copies[3].wait()
    normalise(value.at[pl.ds(half, head - half), :], held.at[pl.ds(half, head - half), :], scale, offset, rows_step)
    hand_out(shards, span, lanes, held, outs)
    for copy in copies[4:]:
        copy.wait()


def rest_kernel(shards, span, rows_step, first, lanes, cuts, gain, bias, value_ref, weight_ref, *refs):
    outs, parts = refs[:len(lanes)], refs[len(lanes):len(lanes) + len(cuts)]
    value, held, sems = refs[len(lanes) + len(cuts):]
    half = value.shape[0] // 32 * 16
    blocks = [pl.ds(0, half), pl.ds(half, value.shape[0] - half)]
    starts = [first, first + half]
    copies = [
        pltpu.make_async_copy(value_ref.at[pl.ds(start, at.size), :], value.at[at, :], sems.at[k])
        for k, (start, at) in enumerate(zip(starts, blocks))
    ]
    copies += weight_copies(cuts, weight_ref, parts, sems, len(copies))
    for copy in copies:
        copy.start()
    scale = gain[...].astype(jnp.float32).reshape(1, -1)
    offset = bias[...].astype(jnp.float32).reshape(1, -1)
    for copy, at in zip(copies, blocks):
        copy.wait()
        normalise(value.at[at, :], held.at[at, :], scale, offset, rows_step)
    hand_out(shards, span, lanes, held, outs)
    for copy in copies[len(blocks):]:
        copy.wait()


def mix_kernel(shards, length, first, start, layout, *refs):
    early, pieces, refs = refs[:shards], refs[shards:2 * shards], refs[2 * shards:]
    weights, refs = refs[:len(layout)], refs[len(layout):]
    bias_ref, outs, (values, mixed) = refs[0], refs[1:1 + shards], refs[1 + shards:]
    here, row = lax.axis_index("sp"), lax.axis_index("dp")
    head = early[0].shape[0]
    rest = pieces[0].shape[0]
    rows = head + rest
    groups = pieces[0].shape[1] // GD
    nblocks = -(-length // BLK)
    for s in range(shards):
        origin = partner(here, s, shards)[1]
        top = pl.multiple_of(origin * rows, GD)
        mixed[pl.ds(top, head), :] = early[s][:, pl.ds(start, groups * GD)]
        mixed[pl.ds(top + head, rest), :] = pieces[s][...]
    for g in range(groups):
        for b in range(nblocks):
            count = min(BLK, length - b * BLK)
            lanes = pl.ds(b * GD, GD)
            values[g, pl.ds(0, count), lanes] = mixed[pl.ds(b * BLK, count), pl.ds(g * GD, GD)]
            if count < BLK:
                values[g, pl.ds(count, BLK - count), lanes] = jnp.zeros((BLK - count, GD), jnp.bfloat16)
    tiles = {}
    for ref, (flip, fixed, low, skip) in zip(weights, layout):
        tiles.setdefault((flip, fixed), []).append((ref, low, skip))
    for (flip, fixed), parts in tiles.items():
        at_row = row ^ flip if fixed is None else fixed
        top = pl.multiple_of(at_row * TILE, TILE)
        for g in range(groups):
            total = None
            for ref, low, skip in parts:
                part = ref[skip + g] if fixed is None else ref[skip + g, pl.ds(fixed * TILE, TILE), :]
                cols = lax.broadcasted_iota(jnp.int32, part.shape, 1) + low
                keep = cols <= lax.broadcasted_iota(jnp.int32, part.shape, 0) + top
                part = jnp.where(keep, part, jnp.zeros_like(part))
                term = jnp.dot(part, values[g, pl.ds(low, part.shape[1]), :], preferred_element_type=jnp.float32)
                total = term if total is None else total + term
            shift = bias_ref[pl.ds(first + g, 1), pl.ds(top, TILE)].astype(jnp.float32)
            shift = jnp.broadcast_to(shift, (GD, TILE)).T
            for b in range(nblocks):
                block = total[:, b * GD:(b + 1) * GD] + shift
                mixed[pl.ds(b * BLK + top, TILE), pl.ds(g * GD, GD)] = block.astype(jnp.bfloat16)
    for s in range(shards):
        target = partner(here, s, shards)[0]
        outs[s][...] = mixed[pl.ds(pl.multiple_of(target * rows, rows), rows), :]


def gate_kernel(shards, chunks, chunk, steps, rows_step, gate_ref, *refs):
    pieces = refs[:len(steps)]
    out_ref, held, sems = refs[-3:]
    here = lax.axis_index("sp")
    width = pieces[0].shape[1]
    copies = []
    parts = sems.shape[1]
    block = gate_ref.shape[0] // parts
    for k, s in enumerate(steps):
        start = (partner(here, s, shards)[1] * chunks + chunk) * width
        lanes = pl.ds(pl.multiple_of(start, GD), width)

        for part in range(parts):

            def step(i, carry, k=k, part=part, lanes=lanes):
                rows = pl.ds(pl.multiple_of(part * block + i * rows_step, rows_step), rows_step)
                gate = 0.5 * twice_gelu(gate_ref[rows, lanes].astype(jnp.float32))
                held[k, rows, :] = (gate * pieces[k][rows, :].astype(jnp.float32)).astype(jnp.bfloat16)
                return carry

            lax.fori_loop(0, block // rows_step, step, 0, unroll=4)
            rows = pl.ds(part * block, block)
            copies.append(pltpu.make_async_copy(held.at[k, rows, :], out_ref.at[rows, lanes], sems.at[k, part]))
            copies[-1].start()
    for copy in copies:
        copy.wait()


def exchange_step(step, x, shards):
    return lax.ppermute(x, "sp", swap_pairs(shards, step))


def exchange_rows(weight, parts, ndp, first):
    got = [(weight[0], 0, None, 0, first), (weight[1], 1, None, 0, first)]
    for low, least, part in parts:
        far = lax.ppermute(part, "dp", [p for p in swap_pairs(ndp, 2) if p[0] >= least])
        got.append((far, 2, None, low, 0))
        got.append((lax.ppermute(far, "dp", swap_pairs(ndp, 1)), 3, None, low, 0))
    return got


def compute(nsp, ndp, exchange, gate, value, gain, bias, mix_weight, mix_bias):
    rows, width = value.shape
    groups = mix_weight.shape[0]
    length = rows * nsp
    chunks = 2 if groups % 2 == 0 else 1
    per = groups // chunks
    nblocks = -(-length // BLK)
    piece = jax.ShapeDtypeStruct((rows, per * GD), jnp.bfloat16)
    small = pltpu.CompilerParams(vmem_limit_bytes=16 << 20)

    columns = [(0, 2 * TILE, 0), (2 * TILE, TILE, 2), (3 * TILE, TILE, 3)] if exchange else []
    cuts = [(c * per, per, low, cols) for c in range(chunks) for low, cols, _ in columns]
    head = rows // 4
    span = groups * GD

    ncuts = min(1, len(cuts))

    def bf16(*shape):
        return jax.ShapeDtypeStruct(shape, jnp.bfloat16)

    def cut_shapes(some):
        return [bf16(n, mix_weight.shape[1], cols) for _, n, _, cols in some]

    def cost(count):
        return pl.CostEstimate(flops=30 * count * width, bytes_accessed=4 * count * width, transcendentals=count * width)

    in_hbm = [pltpu.with_memory_space_constraint(x, pltpu.HBM) for x in (value, gain, bias, mix_weight)]
    lanes = [(s, 0, span) for s in range(nsp)]
    shapes = [bf16(head, span)] * nsp + cut_shapes(cuts[:ncuts]) + [bf16(width), bf16(width)]
    made = pl.pallas_call(
        functools.partial(head_kernel, nsp, span, 16, lanes, cuts[:ncuts]),
        out_shape=shapes,
        in_specs=[HBM] * 4,
        out_specs=[VMEM] * len(shapes),
        scratch_shapes=[
            pltpu.VMEM((head, width), jnp.bfloat16),
            pltpu.VMEM((head, width), jnp.bfloat16),
            pltpu.SemaphoreType.DMA((4 + ncuts,)),
        ],
        compiler_params=small,
        cost_estimate=cost(head),
        name="norm_head",
    )(*in_hbm)
    first_sent, parts, ready = made[:nsp], made[nsp:nsp + ncuts], made[nsp + ncuts:]
    far = {s: exchange_step(s, first_sent[s], nsp) for s in steps_of(nsp)}
    early = [first_sent[0]] + [far[s] for s in range(1, nsp)]
    lanes = [(s, c * per * GD, per * GD) for c in range(chunks) for s in range(nsp)]
    shapes = [bf16(rows - head, per * GD)] * (nsp * chunks) + cut_shapes(cuts[ncuts:])
    made = pl.pallas_call(
        functools.partial(rest_kernel, nsp, span, 16, head, lanes, cuts[ncuts:]),
        out_shape=shapes,
        in_specs=[VMEM] * 2 + [HBM] * 2,
        out_specs=[VMEM] * len(shapes),
        scratch_shapes=[
            pltpu.VMEM((rows - head, width), jnp.bfloat16),
            pltpu.VMEM((rows - head, width), jnp.bfloat16),
            pltpu.SemaphoreType.DMA((2 + len(cuts) - ncuts,)),
        ],
        compiler_params=small,
        cost_estimate=cost(rows - head),
        name="norm_rest",
    )(*ready, in_hbm[0], in_hbm[3])
    sent, parts = made[:nsp * chunks], list(parts) + list(made[nsp * chunks:])
    weights = []
    if exchange:
        other = lax.ppermute(mix_weight, "dp", swap_pairs(ndp, 1))
        for c in range(chunks):
            mine = parts[c * len(columns):(c + 1) * len(columns)]
            mine = [(low, least, part) for (low, _, least), part in zip(columns, mine)]
            weights.append(exchange_rows((mix_weight, other), mine, ndp, c * per))
    else:
        whole = lax.all_gather(mix_weight, "dp", axis=1, tiled=True)
        weights = [[(whole, 0, i, 0, c * per) for i in range(BLK // TILE)] for c in range(chunks)]
    out = None
    got = []
    for c in range(chunks):
        mine = sent[c * nsp:(c + 1) * nsp]
        far = {s: exchange_step(s, mine[s], nsp) for s in steps_of(nsp)}
        got.append([mine[0]] + [far[s] for s in range(1, nsp)])
    backs = []
    for c in range(chunks):
        layout = [w[1:] for w in weights[c]]
        outs = pl.pallas_call(
            functools.partial(mix_kernel, nsp, length, c * per, c * per * GD, layout),
            out_shape=[piece] * nsp,
            in_specs=[VMEM] * (2 * nsp + len(layout) + 1),
            out_specs=[VMEM] * nsp,
            scratch_shapes=[
                pltpu.VMEM((per, BLK, nblocks * GD), jnp.bfloat16),
                pltpu.VMEM((nblocks * BLK, per * GD), jnp.bfloat16),
            ],
            compiler_params=pltpu.CompilerParams(vmem_limit_bytes=24 << 20),
            cost_estimate=pl.CostEstimate(flops=2 * per * BLK * length * GD, bytes_accessed=per * BLK * BLK, transcendentals=0),
        )(*early, *got[c], *[w[0] for w in weights[c]], mix_bias)
        far = {s: exchange_step(s, outs[s], nsp) for s in steps_of(nsp)}
        backs += [[outs[0]] + [far[s] for s in range(1, nsp)]]
    out = None
    order = list(range(nsp))
    calls = [(c, order) for c in range(chunks - 1)] + [(chunks - 1, order[:-1]), (chunks - 1, order[-1:])]
    for c, steps in calls:
        extra = [] if out is None else [out]
        share = rows * per * GD * len(steps)
        out = pl.pallas_call(
            functools.partial(gate_kernel, nsp, chunks, c, steps, 32),
            out_shape=jax.ShapeDtypeStruct((rows, width), jnp.bfloat16),
            in_specs=[VMEM] * (1 + len(steps)) + [HBM] * len(extra),
            out_specs=HBM,
            scratch_shapes=[pltpu.VMEM((len(steps), rows, per * GD), jnp.bfloat16), pltpu.SemaphoreType.DMA((len(steps), 3 if rows % 96 == 0 else 1))],
            input_output_aliases={len(steps) + 1: 0} if extra else {},
            compiler_params=small,
            cost_estimate=pl.CostEstimate(flops=12 * share, bytes_accessed=6 * share, transcendentals=share),
        )(gate, *[backs[c][s] for s in steps], *extra)
    return out


def body(nsp, ndp, exchange, gate_input, value_input, norm_gain, norm_bias, mix_weight, mix_bias):
    outs = [
        compute(nsp, ndp, exchange, gate_input[q], value_input[q], norm_gain, norm_bias, mix_weight, mix_bias)
        for q in range(value_input.shape[0])
    ]
    return jnp.stack(outs)


def solution(mesh):
    nsp, ndp = mesh.shape["sp"], mesh.shape["dp"]
    exchange = ndp == BLK // TILE == 4
    placed = (
        P(("grp", "dp"), "sp", None),
        P(("grp", "dp"), "sp", None),
        P(),
        P(),
        P("sp", "dp", None),
        P("sp", None),
    )
    return jax.shard_map(
        functools.partial(body, nsp, ndp, exchange),
        mesh=mesh,
        in_specs=placed,
        out_specs=P(("grp", "dp"), "sp", None),
        check_vma=False,
    )
```

```python
import functools

import jax
import jax.numpy as jnp
from jax import lax
from jax.experimental import pallas as pl
from jax.experimental.pallas import tpu as pltpu
from jax.sharding import PartitionSpec as P


GD = 128
BLK = 1024
TILE = 256


VMEM = pl.BlockSpec(memory_space=pltpu.VMEM)
HBM = pl.BlockSpec(memory_space=pltpu.HBM)


def twice_gelu(x):
    return x + x * jnp.tanh(x * (0.7978845608028654 + 0.035677408136300125 * (x * x)))


def partner(here, step, shards):
    if shards & (shards - 1) == 0:
        return here ^ step, here ^ step
    return lax.rem(here + step, shards), lax.rem(here + shards - step, shards)


def swap_pairs(count, step):
    if count & (count - 1) == 0:
        return [(i, i ^ step) for i in range(count)]
    return [(i, (i + step) % count) for i in range(count)]


def steps_of(shards):
    return list(range(shards - 1, 0, -1))


def normalise(value, held, scale, offset, rows_step):
    def step(i, carry):
        at = pl.ds(pl.multiple_of(i * rows_step, rows_step), rows_step)
        act = twice_gelu(value[at, :].astype(jnp.float32))
        centred = act - jnp.mean(act, axis=-1, keepdims=True)
        var = jnp.mean(jnp.square(centred), axis=-1, keepdims=True)
        held[at, :] = (centred * lax.rsqrt(var + 4e-06) * scale + offset).astype(jnp.bfloat16)
        return carry

    steps = value.shape[0] // rows_step
    lax.fori_loop(0, steps, step, 0, unroll=next(u for u in (8, 9, 7, 6, 5, 4, 3, 2, 1) if steps % u == 0))


def hand_out(shards, span, lanes, held, outs):
    here = lax.axis_index("sp")
    for out, (s, low, width) in zip(outs, lanes):
        start = pl.multiple_of(partner(here, s, shards)[0] * span + low, GD)
        out[...] = held[:, pl.ds(start, width)]


def weight_copies(cuts, weight_ref, parts, sems, first):
    copies = []
    for k, (part, (group, count, low, cols)) in enumerate(zip(parts, cuts)):
        source = weight_ref.at[pl.ds(group, count), :, pl.ds(low, cols)]
        copies.append(pltpu.make_async_copy(source, part, sems.at[first + k]))
    return copies


def head_kernel(shards, span, rows_step, lanes, cuts, value_ref, gain_ref, bias_ref, weight_ref, *refs):
    outs, parts = refs[:len(lanes)], refs[len(lanes):len(lanes) + len(cuts)]
    gain, bias, value, held, sems = refs[len(lanes) + len(cuts):]
    head = value.shape[0]
    pairs = [
        (value_ref.at[pl.ds(0, head), :], value),
        (gain_ref, gain),
        (bias_ref, bias),
    ]
    copies = [pltpu.make_async_copy(source, target, sems.at[k]) for k, (source, target) in enumerate(pairs)]
    copies += weight_copies(cuts, weight_ref, parts, sems, len(pairs))
    for copy in copies:
        copy.start()
    for copy in copies[:3]:
        copy.wait()
    scale = gain[...].astype(jnp.float32).reshape(1, -1)
    offset = bias[...].astype(jnp.float32).reshape(1, -1)
    normalise(value, held, scale, offset, rows_step)
    hand_out(shards, span, lanes, held, outs)
    for copy in copies[3:]:
        copy.wait()


def rest_kernel(shards, span, rows_step, first, lanes, cuts, gain, bias, value_ref, weight_ref, *refs):
    outs, parts = refs[:len(lanes)], refs[len(lanes):len(lanes) + len(cuts)]
    value, held, sems = refs[len(lanes) + len(cuts):]
    half = value.shape[0] // 32 * 16
    blocks = [pl.ds(0, half), pl.ds(half, value.shape[0] - half)]
    starts = [first, first + half]
    copies = [
        pltpu.make_async_copy(value_ref.at[pl.ds(start, at.size), :], value.at[at, :], sems.at[k])
        for k, (start, at) in enumerate(zip(starts, blocks))
    ]
    copies += weight_copies(cuts, weight_ref, parts, sems, len(copies))
    for copy in copies:
        copy.start()
    scale = gain[...].astype(jnp.float32).reshape(1, -1)
    offset = bias[...].astype(jnp.float32).reshape(1, -1)
    for copy, at in zip(copies, blocks):
        copy.wait()
        normalise(value.at[at, :], held.at[at, :], scale, offset, rows_step)
    hand_out(shards, span, lanes, held, outs)
    for copy in copies[len(blocks):]:
        copy.wait()


def mix_kernel(shards, length, first, start, layout, *refs):
    early, pieces, refs = refs[:shards], refs[shards:2 * shards], refs[2 * shards:]
    weights, refs = refs[:len(layout)], refs[len(layout):]
    bias_ref, outs, (values, mixed) = refs[0], refs[1:1 + shards], refs[1 + shards:]
    here, row = lax.axis_index("sp"), lax.axis_index("dp")
    head = early[0].shape[0]
    rest = pieces[0].shape[0]
    rows = head + rest
    groups = pieces[0].shape[1] // GD
    nblocks = -(-length // BLK)
    for s in range(shards):
        origin = partner(here, s, shards)[1]
        top = pl.multiple_of(origin * rows, GD)
        mixed[pl.ds(top, head), :] = early[s][:, pl.ds(start, groups * GD)]
        mixed[pl.ds(top + head, rest), :] = pieces[s][...]
    for g in range(groups):
        for b in range(nblocks):
            count = min(BLK, length - b * BLK)
            lanes = pl.ds(b * GD, GD)
            values[g, pl.ds(0, count), lanes] = mixed[pl.ds(b * BLK, count), pl.ds(g * GD, GD)]
            if count < BLK:
                values[g, pl.ds(count, BLK - count), lanes] = jnp.zeros((BLK - count, GD), jnp.bfloat16)
    tiles = {}
    for ref, (flip, fixed, low, skip) in zip(weights, layout):
        tiles.setdefault((flip, fixed), []).append((ref, low, skip))
    for (flip, fixed), parts in tiles.items():
        at_row = row ^ flip if fixed is None else fixed
        top = pl.multiple_of(at_row * TILE, TILE)
        for g in range(groups):
            total = None
            for ref, low, skip in parts:
                part = ref[skip + g] if fixed is None else ref[skip + g, pl.ds(fixed * TILE, TILE), :]
                cols = lax.broadcasted_iota(jnp.int32, part.shape, 1) + low
                keep = cols <= lax.broadcasted_iota(jnp.int32, part.shape, 0) + top
                part = jnp.where(keep, part, jnp.zeros_like(part))
                term = jnp.dot(part, values[g, pl.ds(low, part.shape[1]), :], preferred_element_type=jnp.float32)
                total = term if total is None else total + term
            shift = bias_ref[pl.ds(first + g, 1), pl.ds(top, TILE)].astype(jnp.float32)
            shift = jnp.broadcast_to(shift, (GD, TILE)).T
            for b in range(nblocks):
                block = total[:, b * GD:(b + 1) * GD] + shift
                mixed[pl.ds(b * BLK + top, TILE), pl.ds(g * GD, GD)] = block.astype(jnp.bfloat16)
    for s in range(shards):
        target = partner(here, s, shards)[0]
        outs[s][...] = mixed[pl.ds(pl.multiple_of(target * rows, rows), rows), :]


def gate_kernel(shards, chunks, chunk, steps, rows_step, gate_ref, *refs):
    pieces = refs[:len(steps)]
    out_ref, held, sems = refs[-3:]
    here = lax.axis_index("sp")
    width = pieces[0].shape[1]
    copies = []
    parts = sems.shape[1]
    block = gate_ref.shape[0] // parts
    for k, s in enumerate(steps):
        start = (partner(here, s, shards)[1] * chunks + chunk) * width
        lanes = pl.ds(pl.multiple_of(start, GD), width)

        for part in range(parts):

            def step(i, carry, k=k, part=part, lanes=lanes):
                rows = pl.ds(pl.multiple_of(part * block + i * rows_step, rows_step), rows_step)
                gate = 0.5 * twice_gelu(gate_ref[rows, lanes].astype(jnp.float32))
                held[k, rows, :] = (gate * pieces[k][rows, :].astype(jnp.float32)).astype(jnp.bfloat16)
                return carry

            lax.fori_loop(0, block // rows_step, step, 0, unroll=4)
            rows = pl.ds(part * block, block)
            copies.append(pltpu.make_async_copy(held.at[k, rows, :], out_ref.at[rows, lanes], sems.at[k, part]))
            copies[-1].start()
    for copy in copies:
        copy.wait()


def exchange_step(step, x, shards):
    return lax.ppermute(x, "sp", swap_pairs(shards, step))


def exchange_rows(weight, parts, ndp, first):
    got = [(weight[0], 0, None, 0, first), (weight[1], 1, None, 0, first)]
    for low, least, part in parts:
        far = lax.ppermute(part, "dp", [p for p in swap_pairs(ndp, 2) if p[0] >= least])
        got.append((far, 2, None, low, 0))
        got.append((lax.ppermute(far, "dp", swap_pairs(ndp, 1)), 3, None, low, 0))
    return got


def compute(nsp, ndp, exchange, gate, value, gain, bias, mix_weight, mix_bias):
    rows, width = value.shape
    groups = mix_weight.shape[0]
    length = rows * nsp
    chunks = 2 if groups % 2 == 0 else 1
    per = groups // chunks
    nblocks = -(-length // BLK)
    piece = jax.ShapeDtypeStruct((rows, per * GD), jnp.bfloat16)
    small = pltpu.CompilerParams(vmem_limit_bytes=16 << 20)

    columns = [(0, 2 * TILE, 0), (2 * TILE, TILE, 2), (3 * TILE, TILE, 3)] if exchange else []
    cuts = [(c * per, per, low, cols) for c in range(chunks) for low, cols, _ in columns]
    head = rows // 4
    span = groups * GD

    ncuts = min(1, len(cuts))

    def bf16(*shape):
        return jax.ShapeDtypeStruct(shape, jnp.bfloat16)

    def cut_shapes(some):
        return [bf16(n, mix_weight.shape[1], cols) for _, n, _, cols in some]

    def cost(count):
        return pl.CostEstimate(flops=30 * count * width, bytes_accessed=4 * count * width, transcendentals=count * width)

    in_hbm = [pltpu.with_memory_space_constraint(x, pltpu.HBM) for x in (value, gain, bias, mix_weight)]
    lanes = [(s, 0, span) for s in range(nsp)]
    shapes = [bf16(head, span)] * nsp + cut_shapes(cuts[:ncuts]) + [bf16(width), bf16(width)]
    made = pl.pallas_call(
        functools.partial(head_kernel, nsp, span, 16, lanes, cuts[:ncuts]),
        out_shape=shapes,
        in_specs=[HBM] * 4,
        out_specs=[VMEM] * len(shapes),
        scratch_shapes=[
            pltpu.VMEM((head, width), jnp.bfloat16),
            pltpu.VMEM((head, width), jnp.bfloat16),
            pltpu.SemaphoreType.DMA((3 + ncuts,)),
        ],
        compiler_params=small,
        cost_estimate=cost(head),
        name="norm_head",
    )(*in_hbm)
    first_sent, parts, ready = made[:nsp], made[nsp:nsp + ncuts], made[nsp + ncuts:]
    far = {s: exchange_step(s, first_sent[s], nsp) for s in steps_of(nsp)}
    early = [first_sent[0]] + [far[s] for s in range(1, nsp)]
    lanes = [(s, c * per * GD, per * GD) for c in range(chunks) for s in range(nsp)]
    shapes = [bf16(rows - head, per * GD)] * (nsp * chunks) + cut_shapes(cuts[ncuts:])
    made = pl.pallas_call(
        functools.partial(rest_kernel, nsp, span, 16, head, lanes, cuts[ncuts:]),
        out_shape=shapes,
        in_specs=[VMEM] * 2 + [HBM] * 2,
        out_specs=[VMEM] * len(shapes),
        scratch_shapes=[
            pltpu.VMEM((rows - head, width), jnp.bfloat16),
            pltpu.VMEM((rows - head, width), jnp.bfloat16),
            pltpu.SemaphoreType.DMA((2 + len(cuts) - ncuts,)),
        ],
        compiler_params=small,
        cost_estimate=cost(rows - head),
        name="norm_rest",
    )(*ready, in_hbm[0], in_hbm[3])
    sent, parts = made[:nsp * chunks], list(parts) + list(made[nsp * chunks:])
    weights = []
    if exchange:
        other = lax.ppermute(mix_weight, "dp", swap_pairs(ndp, 1))
        for c in range(chunks):
            mine = parts[c * len(columns):(c + 1) * len(columns)]
            mine = [(low, least, part) for (low, _, least), part in zip(columns, mine)]
            weights.append(exchange_rows((mix_weight, other), mine, ndp, c * per))
    else:
        whole = lax.all_gather(mix_weight, "dp", axis=1, tiled=True)
        weights = [[(whole, 0, i, 0, c * per) for i in range(BLK // TILE)] for c in range(chunks)]
    out = None
    got = []
    for c in range(chunks):
        mine = sent[c * nsp:(c + 1) * nsp]
        far = {s: exchange_step(s, mine[s], nsp) for s in steps_of(nsp)}
        got.append([mine[0]] + [far[s] for s in range(1, nsp)])
    backs = []
    for c in range(chunks):
        layout = [w[1:] for w in weights[c]]
        outs = pl.pallas_call(
            functools.partial(mix_kernel, nsp, length, c * per, c * per * GD, layout),
            out_shape=[piece] * nsp,
            in_specs=[VMEM] * (2 * nsp + len(layout) + 1),
            out_specs=[VMEM] * nsp,
            scratch_shapes=[
                pltpu.VMEM((per, BLK, nblocks * GD), jnp.bfloat16),
                pltpu.VMEM((nblocks * BLK, per * GD), jnp.bfloat16),
            ],
            compiler_params=pltpu.CompilerParams(vmem_limit_bytes=24 << 20),
            cost_estimate=pl.CostEstimate(flops=2 * per * BLK * length * GD, bytes_accessed=per * BLK * BLK, transcendentals=0),
        )(*early, *got[c], *[w[0] for w in weights[c]], mix_bias)
        far = {s: exchange_step(s, outs[s], nsp) for s in steps_of(nsp)}
        backs += [[outs[0]] + [far[s] for s in range(1, nsp)]]
    out = None
    order = list(range(nsp))
    calls = [(c, order) for c in range(chunks - 1)] + [(chunks - 1, order[:-1]), (chunks - 1, order[-1:])]
    for c, steps in calls:
        extra = [] if out is None else [out]
        share = rows * per * GD * len(steps)
        out = pl.pallas_call(
            functools.partial(gate_kernel, nsp, chunks, c, steps, 32),
            out_shape=jax.ShapeDtypeStruct((rows, width), jnp.bfloat16),
            in_specs=[VMEM] * (1 + len(steps)) + [HBM] * len(extra),
            out_specs=HBM,
            scratch_shapes=[pltpu.VMEM((len(steps), rows, per * GD), jnp.bfloat16), pltpu.SemaphoreType.DMA((len(steps), 3 if rows % 96 == 0 else 1))],
            input_output_aliases={len(steps) + 1: 0} if extra else {},
            compiler_params=small,
            cost_estimate=pl.CostEstimate(flops=12 * share, bytes_accessed=6 * share, transcendentals=share),
        )(gate, *[backs[c][s] for s in steps], *extra)
    return out


def body(nsp, ndp, exchange, gate_input, value_input, norm_gain, norm_bias, mix_weight, mix_bias):
    outs = [
        compute(nsp, ndp, exchange, gate_input[q], value_input[q], norm_gain, norm_bias, mix_weight, mix_bias)
        for q in range(value_input.shape[0])
    ]
    return jnp.stack(outs)


def solution(mesh):
    nsp, ndp = mesh.shape["sp"], mesh.shape["dp"]
    exchange = ndp == BLK // TILE == 4
    placed = (
        P(("grp", "dp"), "sp", None),
        P(("grp", "dp"), "sp", None),
        P(),
        P(),
        P("sp", "dp", None),
        P("sp", None),
    )
    return jax.shard_map(
        functools.partial(body, nsp, ndp, exchange),
        mesh=mesh,
        in_specs=placed,
        out_specs=P(("grp", "dp"), "sp", None),
        check_vma=False,
    )
```
